32 devices in a mesh: ep: 32 (over z, y, x, core).
Axes of the slice: x: 2, y: 2, z: 4, core: 2. Of those that a mesh axis runs over, the one named last changes fastest.
Arguments:
- tokens: bfloat16 [768, 2048], P('ep'), may hold values from -6 to 6
- state: float32 [768, 16, 64, 64], P('ep'), may hold values from -4 to 4
- norm_gain: float32 [2048], replicated, may hold values from 0.1 to 1.9
- w_recept: bfloat16 [2048, 1024], replicated, may hold values from -0.125 to 0.125
- w_keys: bfloat16 [2048, 1024], replicated, may hold values from -0.125 to 0.125
- w_values: bfloat16 [2048, 1024], replicated, may hold values from -0.125 to 0.125
- decay_base: float32 [1024], replicated, may hold values from -3 to 3
- decay_first_matrix: bfloat16 [2048, 128], replicated, may hold values from -0.125 to 0.125
- decay_second_matrix: bfloat16 [128, 1024], replicated, may hold values from -0.5 to 0.5
- rate_base: float32 [1024], replicated, may hold values from -3 to 3
- rate_first_matrix: bfloat16 [2048, 128], replicated, may hold values from -0.125 to 0.125
- rate_second_matrix: bfloat16 [128, 1024], replicated, may hold values from -0.5 to 0.5
- head_gain: float32 [1024], replicated, may hold values from 0.1 to 1.9
- w_output: bfloat16 [1024, 2048], replicated, may hold values from -0.1875 to 0.1875
- second_gain: float32 [2048], replicated, may hold values from 0.1 to 1.9
- route_ids: int32 [768, 2], replicated, may hold values from 0 to 15, all different within a row; in each aligned block of 24 rows (0 to 23, 24 to 47, ...) at most 6 rows name the same one
- route_weights: float32 [768, 2], replicated, may hold values from 0.2 to 1
- expert_gate: bfloat16 [2048, 49152], P(None, 'ep'), may hold values from -0.125 to 0.125
- expert_up: bfloat16 [2048, 49152], P(None, 'ep'), may hold values from -0.125 to 0.125
- expert_down: bfloat16 [49152, 2048], P('ep'), may hold values from -0.109375 to 0.109375
Outputs:
- layer_out: bfloat16 [768, 2048], P('ep')
- new_state: float32 [768, 16, 64, 64], P('ep')
The draws below stay inside these ranges and needn't reach their ends.
Inputs may be any that keep to these rules, and one draw needn't show every extreme that they name: `route_ids`: each row names 2 different experts. Among the 24 rows of one device (aligned blocks), no expert is named by more than 6 rows, and in every draw some block names some expert exactly 6 times.
All inputs are finite; a program needn't handle non-finite values.
Results may differ from the reference program's by a relative error of at most 0.015.
Values may be sent and summed in bfloat16 or wider, within the bound.
A program may use at most 192 MiB of HBM per device.

```python
import math
import jax
import jax.numpy as jnp
import numpy as np
from jax import lax

MODEL_WIDTH = 2048
MIXER_HEADS = 16
HEAD_SIZE = 64
LOWRANK_WIDTH = 128
EXPERTS = 16
FF_E = 3072
TOPK = 2
SEQ_DEV = 24
CAP_DEV = 6
BATCH = 768
N_EP = 32


def levels(stream_key, dims, cuts, least, high):
    def one(axis_at, shards_of):
        heights = jax.random.uniform(jax.random.fold_in(jax.random.fold_in(stream_key, 6), axis_at), (shards_of,), jnp.float32, least / len(cuts), high / len(cuts))
        return jnp.repeat(jnp.exp(heights), dims[axis_at] // shards_of).reshape((-1,) + (1,) * (len(dims) - axis_at - 1))

    level = one(*cuts[0])
    for cut in cuts[1:]:
        level = level * one(*cut)
    return level


def assign_block(key, own, number, rows, amount, top, most, slope):
    order = jax.random.permutation(key, amount)
    heavy_load, usual = portions_of(amount, rows * top, most, slope, True), portions_of(amount, rows * top, most, slope, False)
    places = jnp.arange(amount)

    def named(lengths, turn):
        used = int((lengths > 0).sum())
        fixed = max(1, used // 4)
        moved = fixed + (places - fixed + turn * (used - fixed)) % max(1, amount - fixed)
        return jnp.zeros((amount,), jnp.int32).at[order[jnp.where(places < fixed, places, moved)]].set(jnp.asarray(lengths, jnp.int32))

    lengths = jnp.where(number % 4 == 0, named(heavy_load, number // 4), named(usual, number - number // 4 - 1))
    mixed = jax.random.permutation(jax.random.fold_in(own, 3), amount)
    donor, taker = mixed[0:amount // 2 * 2:2], mixed[1:amount // 2 * 2:2]
    room = jnp.minimum(lengths[donor] - 1, most - lengths[taker]) // 2
    room = jnp.where((donor == order[0]) | (taker == order[0]) | (lengths[taker] == 0), 0, jnp.maximum(room, 0))
    moved = jax.random.randint(jax.random.fold_in(own, 4), (amount // 2,), 0, 1 << 20) % (room + 1)
    lengths = lengths.at[donor].add(-moved).at[taker].add(moved)
    items = jnp.searchsorted(jnp.cumsum(lengths), jnp.arange(rows * top), side="right").astype(jnp.int32)
    table = items.reshape(top, rows).T
    table = table[jax.random.permutation(jax.random.fold_in(own, 1), rows)]
    turn = jax.random.randint(jax.random.fold_in(own, 2), (rows, 1), 0, top)
    return jnp.take_along_axis(table, (jnp.arange(top)[None, :] + turn) % top, axis=1)


def portions_of(number_of, total, most, slope, full):
    loads = [(1 << 20) // math.isqrt(grade ** slope) + 1 for grade in range(1, number_of + 1)]
    largest = most if full else min(most, max(-(-total // number_of), total * loads[0] // sum(loads)))
    least = 1 if total - largest >= number_of - 1 else 0
    counts, rest = [largest] + [least] * (number_of - 1), total - largest - least * (number_of - 1)
    while rest > 0:
        free = [i for i in range(1, number_of) if counts[i] < largest] or [i for i in range(1, number_of) if counts[i] < most]
        pool, left = sum([loads[i] for i in free]), rest
        for i in free:
            addition = min(most - counts[i], max(1, left * loads[i] // pool), rest)
            counts[i] = counts[i] + addition
            rest = rest - addition
    return np.array(counts)


def normal_values(stream_key, dims, scale, bound, cuts=(), held_as=jnp.bfloat16):
    level = levels(stream_key, dims, cuts, -0.22, 0.18) if cuts else 1.0
    values = jax.random.normal(stream_key, dims, jnp.float32) * scale * level
    return jnp.minimum(jnp.maximum(values, -bound), bound).astype(held_as)


def setup_inputs(seed: int = 0) -> dict:
    key_list = jax.random.split(jax.random.key(seed), 21)
    tokens = normal_values(key_list[0], (BATCH, MODEL_WIDTH), 1.0, 6.0, ((0, 32),))
    state = normal_values(key_list[1], (BATCH, MIXER_HEADS, HEAD_SIZE, HEAD_SIZE), 0.5, 4.0, ((0, 32),), jnp.float32)
    norm_gain = jnp.clip(1.0 + 0.18 * jax.random.normal(key_list[2], (MODEL_WIDTH,), jnp.float32), 0.1, 1.9)
    w_recept = normal_values(key_list[3], (MODEL_WIDTH, MIXER_HEADS * HEAD_SIZE), MODEL_WIDTH ** -0.5, 0.125)
    w_keys = normal_values(key_list[4], (MODEL_WIDTH, MIXER_HEADS * HEAD_SIZE), MODEL_WIDTH ** -0.5, 0.125)
    w_values = normal_values(key_list[5], (MODEL_WIDTH, MIXER_HEADS * HEAD_SIZE), MODEL_WIDTH ** -0.5, 0.125)
    decay_base = normal_values(key_list[6], (MIXER_HEADS * HEAD_SIZE,), 1.0, 3.0, (), jnp.float32)
    decay_first_matrix = normal_values(key_list[7], (MODEL_WIDTH, LOWRANK_WIDTH), MODEL_WIDTH ** -0.5, 0.125)
    decay_second_matrix = normal_values(key_list[8], (LOWRANK_WIDTH, MIXER_HEADS * HEAD_SIZE), LOWRANK_WIDTH ** -0.5, 0.5)
    rate_base = normal_values(key_list[9], (MIXER_HEADS * HEAD_SIZE,), 1.0, 3.0, (), jnp.float32)
    rate_first_matrix = normal_values(key_list[10], (MODEL_WIDTH, LOWRANK_WIDTH), MODEL_WIDTH ** -0.5, 0.125)
    rate_second_matrix = normal_values(key_list[11], (LOWRANK_WIDTH, MIXER_HEADS * HEAD_SIZE), LOWRANK_WIDTH ** -0.5, 0.5)
    head_gain = jnp.clip(1.0 + 0.18 * jax.random.normal(key_list[12], (MIXER_HEADS * HEAD_SIZE,), jnp.float32), 0.1, 1.9)
    w_output = normal_values(key_list[13], (MIXER_HEADS * HEAD_SIZE, MODEL_WIDTH), (MIXER_HEADS * HEAD_SIZE) ** -0.5, 0.1875)
    second_gain = jnp.clip(1.0 + 0.18 * jax.random.normal(key_list[14], (MODEL_WIDTH,), jnp.float32), 0.1, 1.9)
    route_ids_keys = jax.random.split(jax.random.fold_in(key_list[15], 1), BATCH // SEQ_DEV)
    route_ids_turns = jax.random.permutation(jax.random.fold_in(key_list[15], 3), BATCH // SEQ_DEV)
    route_ids = jax.vmap(lambda own, number: assign_block(jax.random.fold_in(key_list[15], 2), own, number, SEQ_DEV, EXPERTS, TOPK, CAP_DEV, 2))(route_ids_keys, route_ids_turns).reshape((BATCH, TOPK))
    route_weights = jnp.clip(jax.random.uniform(key_list[16], (BATCH, TOPK), jnp.float32, 0.2, 1.0), 0.2, 1.0)
    expert_gate = normal_values(key_list[17], (MODEL_WIDTH, EXPERTS * FF_E), MODEL_WIDTH ** -0.5, 0.125, ((1, 32),))
    expert_up = normal_values(key_list[18], (MODEL_WIDTH, EXPERTS * FF_E), MODEL_WIDTH ** -0.5, 0.125, ((1, 32),))
    expert_down = normal_values(key_list[19], (EXPERTS * FF_E, MODEL_WIDTH), FF_E ** -0.5, 0.109375, ((0, 32),))
    return {"tokens": tokens, "state": state, "norm_gain": norm_gain, "w_recept": w_recept, "w_keys": w_keys, "w_values": w_values, "decay_base": decay_base, "decay_first_matrix": decay_first_matrix, "decay_second_matrix": decay_second_matrix, "rate_base": rate_base, "rate_first_matrix": rate_first_matrix, "rate_second_matrix": rate_second_matrix, "head_gain": head_gain, "w_output": w_output, "second_gain": second_gain, "route_ids": route_ids, "route_weights": route_weights, "expert_gate": expert_gate, "expert_up": expert_up, "expert_down": expert_down}


def norm_rows(values, gain):
    mean_sq = lax.optimization_barrier(jnp.mean(values * values, axis=-1, keepdims=True))
    return values * lax.rsqrt(mean_sq + 1e-06) * gain

def time_mixer(tokens, state, norm_gain, w_recept, w_keys, w_values, decay_base, decay_first_matrix, decay_second_matrix, rate_base, rate_first_matrix, rate_second_matrix, head_gain, w_output):
    count = tokens.shape[0]
    heads = state.shape[1]
    width = state.shape[2]
    resid = tokens.astype(jnp.float32)
    normed = norm_rows(resid, norm_gain).astype(jnp.bfloat16)
    recept = jnp.dot(normed, w_recept, preferred_element_type=jnp.float32).astype(jnp.bfloat16)
    keys = jnp.dot(normed, w_keys, preferred_element_type=jnp.float32).astype(jnp.bfloat16)
    vals = jnp.dot(normed, w_values, preferred_element_type=jnp.float32).astype(jnp.bfloat16)
    decay_low = jnp.tanh(jnp.dot(normed, decay_first_matrix, preferred_element_type=jnp.float32)).astype(jnp.bfloat16)
    rate_low = jnp.dot(normed, rate_first_matrix, preferred_element_type=jnp.float32).astype(jnp.bfloat16)
    pre = decay_base + jnp.dot(decay_low, decay_second_matrix, preferred_element_type=jnp.float32)
    decay = jnp.exp(-jnp.exp(-jax.nn.softplus(-pre) - 0.5))
    rate = jax.nn.sigmoid(rate_base + jnp.dot(rate_low, rate_second_matrix, preferred_element_type=jnp.float32))

    def split_heads(values):
        return values.astype(jnp.float32).reshape(count, heads, width)
    r_head = split_heads(recept)
    k_head = split_heads(keys)
    v_head = split_heads(vals)
    d_head = split_heads(decay)
    a_head = split_heads(rate)
    unit = k_head * lax.rsqrt(lax.optimization_barrier(jnp.sum(k_head * k_head, axis=-1, keepdims=True)) + 1e-06)
    probe = jnp.einsum('bhvk,bhk->bhv', state, unit, precision=lax.Precision.HIGHEST)
    updated = state * d_head[:, :, None, :] - probe[..., None] * (unit * a_head)[:, :, None, :] + v_head[..., None] * k_head[:, :, None, :]
    mixed = jnp.einsum('bhvk,bhk->bhv', updated, r_head, precision=lax.Precision.HIGHEST)
    centre = mixed - lax.optimization_barrier(jnp.mean(mixed, axis=-1, keepdims=True))
    spread = lax.optimization_barrier(jnp.mean(centre * centre, axis=-1, keepdims=True))
    mixed = centre * lax.rsqrt(spread + 0.00064)
    mixed = (mixed.reshape(count, heads * width) * head_gain).astype(jnp.bfloat16)
    after = resid + jnp.dot(mixed, w_output, preferred_element_type=jnp.float32)
    return (after, updated)

def expert_part(rows, gate_w, up_w, down_w):
    gate = jnp.dot(rows, gate_w, preferred_element_type=jnp.float32)
    upper = jnp.dot(rows, up_w, preferred_element_type=jnp.float32)
    hidden = (jax.nn.silu(gate) * upper).astype(jnp.bfloat16)
    return jnp.dot(hidden, down_w, preferred_element_type=jnp.float32)

def reference(tokens, state, norm_gain, w_recept, w_keys, w_values, decay_base, decay_first_matrix, decay_second_matrix, rate_base, rate_first_matrix, rate_second_matrix, head_gain, w_output, second_gain, route_ids, route_weights, expert_gate, expert_up, expert_down):
    blocks_tok = tokens.reshape(N_EP, SEQ_DEV, MODEL_WIDTH)
    blocks_state = state.reshape((N_EP, SEQ_DEV) + state.shape[1:])

    def one_block(pair):
        return time_mixer(pair[0], pair[1], norm_gain, w_recept, w_keys, w_values, decay_base, decay_first_matrix, decay_second_matrix, rate_base, rate_first_matrix, rate_second_matrix, head_gain, w_output)
    after, new_state = lax.map(one_block, (blocks_tok, blocks_state))
    after = after.reshape(BATCH, MODEL_WIDTH)
    new_state = new_state.reshape(state.shape)
    second = norm_rows(after, second_gain).astype(jnp.bfloat16)
    gates_all = expert_gate.reshape(MODEL_WIDTH, EXPERTS, FF_E).transpose(1, 0, 2)
    ups_all = expert_up.reshape(MODEL_WIDTH, EXPERTS, FF_E).transpose(1, 0, 2)
    downs_all = expert_down.reshape(EXPERTS, FF_E, MODEL_WIDTH)
    limit = N_EP * CAP_DEV

    def one_expert(total, inputs):
        which, gate_w, up_w, down_w = inputs
        hit = route_ids == which
        member = jnp.any(hit, axis=1)
        share = lax.optimization_barrier(jnp.sum(jnp.where(hit, route_weights, 0.0), axis=1))
        picked = jnp.nonzero(member, size=limit, fill_value=0)[0].astype(jnp.int32)
        valid = (jnp.arange(limit, dtype=jnp.int32) < jnp.sum(member.astype(jnp.int32))).astype(jnp.float32)
        result = expert_part(second[picked], gate_w, up_w, down_w)
        total = total.at[picked].add((share[picked] * valid)[:, None] * result)
        return (total, None)
    blend, _ = lax.scan(one_expert, jnp.zeros((BATCH, MODEL_WIDTH), jnp.float32), (jnp.arange(EXPERTS, dtype=jnp.int32), gates_all, ups_all, downs_all))
    layer_out = (after + blend).astype(jnp.bfloat16)
    return (layer_out, new_state)
```

```python
import functools
import math

import jax
import jax.numpy as jnp
from jax import lax
from jax.experimental import pallas as pl
from jax.experimental.pallas import tpu as pltpu
from jax.sharding import PartitionSpec as P

EXPERTS = 16
CAP_DEV = 6
ROWS = 8
PARTS = 3
MESH = pl.DeviceIdType.MESH
BF = jnp.bfloat16
F32 = jnp.float32


def dot(a, b):
    return jnp.dot(a, b, preferred_element_type=F32)


def mixer_kernel(
    tokens, norm_gain, decay_base, rate_base, head_gain, second_gain, table,
    state, w_recept, w_keys, w_values, d_first, d_second, r_first, r_second, w_output,
    new_state, after_ref, packed_ref,
    st, wr, wk, wv, df, ds, rf, rs, wo, kh, rh, dh, ah, vt, mt,
    w_sem, in_sem, out_sem,
):
    count, heads, width, _ = state.shape
    loads = [
        pltpu.make_async_copy(src, dst, w_sem.at[i])
        for i, (src, dst) in enumerate(
            [
                (d_first, df), (r_first, rf), (w_keys, wk), (w_values, wv), (d_second, ds),
                (r_second, rs), (w_recept, wr), (w_output, wo),
            ]
        )
    ]
    for copy in loads[:7]:
        copy.start()

    def fetch(h):
        return pltpu.make_async_copy(state.at[:, h], st.at[h], in_sem.at[h])

    def put(h):
        return pltpu.make_async_copy(st.at[h], new_state.at[:, h], out_sem.at[h])

    def start_fetch(h, c):
        fetch(h).start()
        return c

    lax.fori_loop(0, heads, start_fetch, 0)
    loads[7].start()

    resid = tokens[...].astype(F32)
    mean_sq = jnp.mean(resid * resid, axis=-1, keepdims=True)
    normed = (resid * lax.rsqrt(mean_sq + 1e-06) * norm_gain[...]).astype(BF)

    def spread(ref, values):
        for h in range(heads):
            ref[h] = values[:, h * width:(h + 1) * width]

    loads[0].wait()
    decay_low = jnp.tanh(dot(normed, df[...])).astype(BF)
    loads[1].wait()
    rate_low = dot(normed, rf[...]).astype(BF)
    loads[2].wait()
    spread(kh, dot(normed, wk[...]).astype(BF).astype(F32))
    loads[3].wait()
    vals = dot(normed, wv[...]).astype(BF).astype(F32)
    lanes = vt.shape[1]
    vt[...] = jnp.concatenate(
        [vals, jnp.zeros((lanes - count, vals.shape[1]), F32)], axis=0
    ).T
    loads[4].wait()
    pre = decay_base[...] + dot(decay_low, ds[...])
    spread(dh, jnp.exp(-jax.nn.sigmoid(pre) * math.exp(-0.5)))
    loads[5].wait()
    spread(ah, jax.nn.sigmoid(rate_base[...] + dot(rate_low, rs[...])))
    loads[6].wait()
    spread(rh, dot(normed, wr[...]).astype(BF).astype(F32))

    def one_head(h, c):
        fetch(h).wait()
        k = kh[h]
        r = rh[h]
        d = dh[h]
        unit = k * lax.rsqrt(jnp.sum(k * k, axis=-1, keepdims=True) + 1e-06)
        ua = unit * ah[h]
        rows = pl.ds(pl.multiple_of(h * width, width), width)
        v = vt[rows, :]
        lane = lax.broadcasted_iota(jnp.int32, (width, lanes), 1)
        mixed = jnp.zeros((width, lanes), F32)
        for b in range(count):
            s = st[h, b]
            probe = jnp.sum(s * unit[b:b + 1], axis=-1, keepdims=True)
            new = s * d[b:b + 1] - probe * ua[b:b + 1] + v[:, b:b + 1] * k[b:b + 1]
            st[h, b] = new
            got = jnp.sum(new * r[b:b + 1], axis=-1, keepdims=True)
            mixed = jnp.where(lane == b, got, mixed)
        put(h).start()
        centre = mixed - jnp.mean(mixed, axis=0, keepdims=True)
        var = jnp.mean(centre * centre, axis=0, keepdims=True)
        mt[rows, :] = centre * lax.rsqrt(var + 0.00064)
        return c

    lax.fori_loop(0, heads, one_head, 0)
    mixed = (mt[...].T[:count] * head_gain[...]).astype(BF)
    loads[7].wait()
    after = resid + dot(mixed, wo[...])
    after_ref[...] = after
    mean_sq = jnp.mean(after * after, axis=-1, keepdims=True)
    second = (after * lax.rsqrt(mean_sq + 1e-06) * second_gain[...]).astype(BF)
    part = second.shape[1] // (PARTS + 1)
    last = second[:, PARTS * part:]
    for j in range(PARTS):
        value = dot(table[PARTS], second[:, j * part:(j + 1) * part]) + dot(table[j], last)
        packed_ref[:, :, j * part:(j + 1) * part] = value.reshape(EXPERTS, ROWS, part).astype(BF)

    def end_put(h, c):
        put(h).wait()
        return c

    lax.fori_loop(0, heads, end_put, 0)


def mixer(args, table):
    (tokens, state, norm_gain, w_recept, w_keys, w_values, decay_base, d_first, d_second,
     rate_base, r_first, r_second, head_gain, w_output, second_gain) = args
    count, heads, width, _ = state.shape
    model = tokens.shape[1]
    part = model // (PARTS + 1)
    lanes = -(-count // 128) * 128
    vm = pl.BlockSpec(memory_space=pltpu.VMEM)
    hb = pl.BlockSpec(memory_space=pl.ANY)
    weights = [w_recept, w_keys, w_values, d_first, d_second, r_first, r_second, w_output]
    head_buf = pltpu.VMEM((heads, count, width), F32)
    return pl.pallas_call(
        mixer_kernel,
        out_shape=(
            jax.ShapeDtypeStruct(state.shape, F32),
            jax.ShapeDtypeStruct((count, model), F32),
            jax.ShapeDtypeStruct((EXPERTS, ROWS, PARTS * part), BF),
        ),
        in_specs=[vm] * 7 + [hb] * 9,
        out_specs=(hb, vm, vm),
        scratch_shapes=[
            pltpu.VMEM((heads, count, width, width), F32),
            *[pltpu.VMEM(w.shape, w.dtype) for w in weights],
            head_buf, head_buf, head_buf, head_buf,
            pltpu.VMEM((heads * width, lanes), F32),
            pltpu.VMEM((heads * width, lanes), F32),
            pltpu.SemaphoreType.DMA((8,)),
            pltpu.SemaphoreType.DMA((heads,)),
            pltpu.SemaphoreType.DMA((heads,)),
        ],
        compiler_params=pltpu.CompilerParams(vmem_limit_bytes=56 * 1024 * 1024),
        name="mixer",
    )(
        tokens, norm_gain[None], decay_base[None], rate_base[None], head_gain[None],
        second_gain[None], table, state, *weights,
    )


def expert_kernel(
    devices, packed, after, blend_w, unpack_m, pack_m, gate_h, up_h, down_h,
    out_ref,
    buf, rows_x, hidden, part_f, part_b, peer_b, zsend, ret, gate, up, down,
    w_sem, send1, recv1, fsend, frecv, ysend, yrecv, rsend, rrecv, own_sem,
):
    group = devices // EXPERTS
    me = lax.axis_index("ep")
    mine = me // group
    place = lax.rem(me, group)
    model = after.shape[1]
    part = model // (PARTS + 1)
    inner = gate.shape[1]
    step = math.gcd(inner, 256)

    loads = [
        pltpu.make_async_copy(src, dst, w_sem.at[i])
        for i, (src, dst) in enumerate([(gate_h, gate), (up_h, up), (down_h, down)])
    ]
    barrier = pltpu.get_barrier_semaphore()

    def other(i):
        return lax.rem(mine + i, EXPERTS)

    def peer(i):
        return lax.rem(place + i, group)

    def greet(i, c):
        pl.semaphore_signal(
            barrier, inc=1, device_id=(other(i) * group + place,), device_id_type=MESH
        )
        return c

    lax.fori_loop(1, EXPERTS, greet, 0)
    for i in range(1, group):
        pl.semaphore_signal(
            barrier, inc=1, device_id=(mine * group + peer(i),), device_id_type=MESH
        )
    for copy in loads:
        copy.start()
    pl.semaphore_wait(barrier, EXPERTS - 1 + group - 1)

    def dispatch(i):
        e = other(i)
        return pltpu.make_async_remote_copy(
            src_ref=packed.at[e], dst_ref=buf.at[place, mine],
            send_sem=send1.at[e], recv_sem=recv1.at[mine],
            device_id=(e * group + place,), device_id_type=MESH,
        )

    def arrive(s):
        return pltpu.make_async_remote_copy(
            src_ref=packed.at[s], dst_ref=buf.at[place, s],
            send_sem=send1.at[s], recv_sem=recv1.at[s],
            device_id=(s * group + place,), device_id_type=MESH,
        )

    def forward(s, i, src):
        q = peer(i)
        return pltpu.make_async_remote_copy(
            src_ref=src, dst_ref=buf.at[place, s],
            send_sem=fsend.at[i, s], recv_sem=frecv.at[place, s],
            device_id=(mine * group + q,), device_id_type=MESH,
        )

    def forwarded(s, i):
        q = peer(i)
        return pltpu.make_async_remote_copy(
            src_ref=buf.at[q, s], dst_ref=buf.at[q, s],
            send_sem=fsend.at[i, s], recv_sem=frecv.at[q, s],
            device_id=(mine * group + q,), device_id_type=MESH,
        )

    def start_dispatch(i, c):
        dispatch(i).start()
        return c

    lax.fori_loop(1, EXPERTS, start_dispatch, 0)
    own = pltpu.make_async_copy(packed.at[mine], buf.at[place, mine], own_sem.at[0])
    own.start()
    for i in range(1, group):
        forward(mine, i, packed.at[mine]).start()

    def relay(j, c):
        s = lax.rem(mine + EXPERTS - j, EXPERTS)
        arrive(s).wait_recv()
        for i in range(1, group):
            forward(s, i, buf.at[place, s]).start()
        return c

    lax.fori_loop(1, EXPERTS, relay, 0)
    own.wait()

    def end_relay(j, c):
        s = lax.rem(mine + EXPERTS - j, EXPERTS)
        for i in range(1, group):
            forwarded(s, i).wait_recv()
        return c

    lax.fori_loop(0, EXPERTS, end_relay, 0)

    packed_rows = EXPERTS * ROWS
    rows = EXPERTS * CAP_DEV
    for q in range(group):
        tail = jnp.zeros((rows, part), F32)
        for j in range(PARTS):
            cols = slice(j * part, (j + 1) * part)
            block = buf[q, :, :, cols].astype(F32).reshape(packed_rows, part).astype(BF)
            rows_x[q * rows:(q + 1) * rows, cols] = dot(unpack_m[PARTS], block).astype(BF)
            tail = tail + dot(unpack_m[j], block)
        rows_x[q * rows:(q + 1) * rows, PARTS * part:] = tail.astype(BF)

    loads[0].wait()
    loads[1].wait()

    def up_step(t, c):
        cols = pl.ds(pl.multiple_of(t * step, step), step)
        g = dot(rows_x[...], gate[:, cols])
        u = dot(rows_x[...], up[:, cols])
        hidden[:, cols] = (g * jax.nn.sigmoid(g) * u).astype(BF)
        return c

    lax.fori_loop(0, inner // step, up_step, 0)
    loads[2].wait()
    wide = math.gcd(model, 256)

    def down_step(t, c):
        cols = pl.ds(pl.multiple_of(t * wide, wide), wide)
        y = dot(hidden[...], down[:, cols])
        for q in range(group):
            mine_rows = y[q * rows:(q + 1) * rows]
            part_f[q, :, cols] = mine_rows
            part_b[q, :, cols] = mine_rows.astype(BF)
        return c

    lax.fori_loop(0, model // wide, down_step, 0)

    def swap(i):
        q = peer(i)
        return pltpu.make_async_remote_copy(
            src_ref=part_b.at[q], dst_ref=peer_b.at[place],
            send_sem=ysend.at[q], recv_sem=yrecv.at[place],
            device_id=(mine * group + q,), device_id_type=MESH,
        )

    def swapped(i):
        q = peer(i)
        return pltpu.make_async_remote_copy(
            src_ref=part_b.at[q], dst_ref=peer_b.at[q],
            send_sem=ysend.at[q], recv_sem=yrecv.at[q],
            device_id=(mine * group + q,), device_id_type=MESH,
        )

    for i in range(1, group):
        swap(i).start()
    for i in range(1, group):
        swapped(i).wait_recv()

    def summed(cols):
        total = part_f[place, :, cols]
        for i in range(1, group):
            total = total + peer_b[peer(i), :, cols].astype(F32)
        return total.astype(BF)

    last = summed(slice(PARTS * part, model))
    for j in range(PARTS):
        cols = slice(j * part, (j + 1) * part)
        value = dot(pack_m[PARTS], summed(cols)) + dot(pack_m[j], last)
        zsend[:, :, cols] = value.reshape(EXPERTS, ROWS, part).astype(BF)

    def give(i):
        e = other(i)
        return pltpu.make_async_remote_copy(
            src_ref=zsend.at[e], dst_ref=ret.at[mine],
            send_sem=rsend.at[e], recv_sem=rrecv.at[mine],
            device_id=(e * group + place,), device_id_type=MESH,
        )

    def take(s):
        return pltpu.make_async_remote_copy(
            src_ref=zsend.at[s], dst_ref=ret.at[s],
            send_sem=rsend.at[s], recv_sem=rrecv.at[s],
            device_id=(s * group + place,), device_id_type=MESH,
        )

    def start_give(i, c):
        give(i).start()
        return c

    lax.fori_loop(1, EXPERTS, start_give, 0)
    own_back = pltpu.make_async_copy(zsend.at[mine], ret.at[mine], own_sem.at[1])
    own_back.start()

    def drain(i, c):
        dispatch(i).wait_send()
        s = lax.rem(mine + EXPERTS - i, EXPERTS)
        for k in range(1, group):
            forwarded(s, k).wait_send()
        return c

    lax.fori_loop(1, EXPERTS, drain, 0)
    for i in range(1, group):
        forwarded(mine, i).wait_send()
        swap(i).wait_send()
    own_back.wait()

    def end_take(j, c):
        take(lax.rem(mine + EXPERTS - j, EXPERTS)).wait_recv()
        return c

    lax.fori_loop(1, EXPERTS, end_take, 0)

    high = blend_w[...].astype(BF)
    low = (blend_w[...] - high.astype(F32)).astype(BF)
    tail = after[:, PARTS * part:]
    for j in range(PARTS):
        cols = slice(j * part, (j + 1) * part)
        block = ret[:, :, cols].astype(F32).reshape(packed_rows, part).astype(BF)
        value = after[:, cols] + dot(high[PARTS], block) + dot(low[PARTS], block)
        out_ref[:, cols] = value.astype(BF)
        tail = tail + dot(high[j], block) + dot(low[j], block)
    out_ref[:, PARTS * part:] = tail.astype(BF)

    def end_give(i, c):
        give(i).wait_send()
        return c

    lax.fori_loop(1, EXPERTS, end_give, 0)


def experts(packed, after, blend_w, gate, up, down, devices):
    group = devices // EXPERTS
    count, model = after.shape
    inner = gate.shape[1]
    rows = EXPERTS * CAP_DEV
    row = jnp.arange(rows)[:, None]
    place = jnp.arange(EXPERTS * ROWS)[None, :]
    same = row // CAP_DEV == place // ROWS
    slot, at = row % CAP_DEV, place % ROWS
    maps = [
        same & (at == CAP_DEV + slot // PARTS) & (slot % PARTS == j) for j in range(PARTS)
    ] + [same & (at == slot)]
    unpack_m = jnp.stack(maps).astype(BF)
    pack_m = unpack_m.transpose(0, 2, 1)
    vm = pl.BlockSpec(memory_space=pltpu.VMEM)
    hb = pl.BlockSpec(memory_space=pl.ANY)
    wide = packed.shape[2]
    dma = pltpu.SemaphoreType.DMA
    return pl.pallas_call(
        functools.partial(expert_kernel, devices),
        out_shape=jax.ShapeDtypeStruct((count, model), BF),
        in_specs=[vm] * 5 + [hb] * 3,
        out_specs=vm,
        scratch_shapes=[
            pltpu.VMEM((group, EXPERTS, ROWS, wide), BF),
            pltpu.VMEM((group * rows, model), BF),
            pltpu.VMEM((group * rows, inner), BF),
            pltpu.VMEM((group, rows, model), F32),
            pltpu.VMEM((group, rows, model), BF),
            pltpu.VMEM((group, rows, model), BF),
            pltpu.VMEM((EXPERTS, ROWS, wide), BF),
            pltpu.VMEM((EXPERTS, ROWS, wide), BF),
            pltpu.VMEM(gate.shape, BF),
            pltpu.VMEM(up.shape, BF),
            pltpu.VMEM(down.shape, BF),
            dma((3,)),
            dma((EXPERTS,)),
            dma((EXPERTS,)),
            dma((group, EXPERTS)),
            dma((group, EXPERTS)),
            dma((group,)),
            dma((group,)),
            dma((EXPERTS,)),
            dma((EXPERTS,)),
            dma((2,)),
        ],
        compiler_params=pltpu.CompilerParams(
            collective_id=0, has_side_effects=True, vmem_limit_bytes=56 * 1024 * 1024
        ),
        name="experts",
    )(packed, after, blend_w, unpack_m, pack_m, gate, up, down)


def tables(route_ids, route_weights, rows_dev):
    start = lax.axis_index("ep") * rows_dev
    ids = lax.dynamic_slice_in_dim(route_ids, start, rows_dev, 0)
    weights = lax.dynamic_slice_in_dim(route_weights, start, rows_dev, 0)
    hit = ids[None, :, :] == jnp.arange(EXPERTS, dtype=jnp.int32)[:, None, None]
    member = jnp.any(hit, axis=2)
    share = jnp.sum(jnp.where(hit, weights[None, :, :], 0.0), axis=2)
    order = jnp.cumsum(member.astype(jnp.int32), axis=1) - 1
    order = jnp.where(member, order, -1)[None, :, None, :]
    at = jnp.arange(ROWS, dtype=jnp.int32)[None, None, :, None]
    piece = jnp.arange(PARTS + 1, dtype=jnp.int32)[:, None, None, None]
    base = jnp.where(
        piece == PARTS,
        jnp.where(at < CAP_DEV, at, -2),
        jnp.where(at >= CAP_DEV, (at - CAP_DEV) * PARTS + piece, -2),
    )
    table = (order == base).astype(F32)
    blend = table * share[None, :, None, :]
    flat = (PARTS + 1, EXPERTS * ROWS, rows_dev)
    return table.reshape(flat).astype(BF), blend.reshape(flat).transpose(0, 2, 1)


def on_device(
    tokens, state, norm_gain, w_recept, w_keys, w_values, decay_base, decay_first_matrix,
    decay_second_matrix, rate_base, rate_first_matrix, rate_second_matrix, head_gain, w_output,
    second_gain, route_ids, route_weights, expert_gate, expert_up, expert_down,
):
    devices = lax.axis_size("ep")
    table, blend_w = tables(route_ids, route_weights, tokens.shape[0])
    new_state, after, packed = mixer(
        (tokens, state, norm_gain, w_recept, w_keys, w_values, decay_base, decay_first_matrix,
         decay_second_matrix, rate_base, rate_first_matrix, rate_second_matrix, head_gain,
         w_output, second_gain),
        table,
    )
    layer_out = experts(packed, after, blend_w, expert_gate, expert_up, expert_down, devices)
    return (layer_out, new_state)


def solution(mesh):
    rep = P()
    in_specs = (
        P("ep", None), P("ep", None, None, None), *[rep] * 15,
        P(None, "ep"), P(None, "ep"), P("ep", None),
    )
    out_specs = (P("ep", None), P("ep", None, None, None))
    return jax.shard_map(
        on_device, mesh=mesh, in_specs=in_specs, out_specs=out_specs, check_vma=False
    )
```

```python
import functools
import math

import jax
import jax.numpy as jnp
import numpy as np
from jax import lax
from jax.experimental import pallas as pl
from jax.experimental.pallas import tpu as pltpu
from jax.sharding import PartitionSpec as P

EXPERTS = 16
CAP_DEV = 6
ROWS = 8
PARTS = 3
MESH = pl.DeviceIdType.MESH
BF = jnp.bfloat16
F32 = jnp.float32


def dot(a, b):
    return jnp.dot(a, b, preferred_element_type=F32)


def mixer_kernel(
    tokens, norm_gain, decay_base, rate_base, head_gain, second_gain, table,
    state, w_recept, w_keys, w_values, d_first, d_second, r_first, r_second, w_output,
    new_state, after_ref, packed_ref,
    st, wr, wk, wv, df, ds, rf, rs, wo, kh, dh, ah, vt, rt, mt,
    w_sem, in_sem, out_sem,
):
    count, heads, width, _ = state.shape
    loads = [
        pltpu.make_async_copy(src, dst, w_sem.at[i])
        for i, (src, dst) in enumerate(
            [
                (d_first, df), (r_first, rf), (w_keys, wk), (w_values, wv), (d_second, ds),
                (r_second, rs), (w_recept, wr), (w_output, wo),
            ]
        )
    ]
    for copy in loads[:7]:
        copy.start()

    def fetch(h):
        return pltpu.make_async_copy(state.at[:, h], st.at[h], in_sem.at[h])

    def put(h):
        return pltpu.make_async_copy(st.at[h], new_state.at[:, h], out_sem.at[h])

    def start_fetch(h, c):
        fetch(h).start()
        return c

    def start_fetches(turn_at):
        low, high = turn_at * heads // 3, (turn_at + 1) * heads // 3
        lax.fori_loop(low, high, start_fetch, 0)

    resid = tokens[...].astype(F32)
    mean_sq = jnp.mean(resid * resid, axis=-1, keepdims=True)
    normed = (resid * lax.rsqrt(mean_sq + 1e-06) * norm_gain[...]).astype(BF)

    def spread(ref, values):
        for h in range(heads):
            ref[h] = values[:, h * width:(h + 1) * width]

    lanes = vt.shape[1]

    def turn(values):
        blank = jnp.zeros((lanes - count, values.shape[1]), F32)
        return jnp.concatenate([values, blank], axis=0).T

    loads[0].wait()
    decay_low = jnp.tanh(dot(normed, df[...])).astype(BF)
    loads[1].wait()
    rate_low = dot(normed, rf[...]).astype(BF)
    loads[2].wait()
    spread(kh, dot(normed, wk[...]).astype(BF).astype(F32))
    start_fetches(0)
    loads[3].wait()
    vals = dot(normed, wv[...]).astype(BF).astype(F32)
    vt[...] = turn(vals)
    start_fetches(1)
    loads[4].wait()
    pre = decay_base[...] + dot(decay_low, ds[...])
    spread(dh, jnp.exp(-jax.nn.sigmoid(pre) * math.exp(-0.5)))
    loads[5].wait()
    spread(ah, jax.nn.sigmoid(rate_base[...] + dot(rate_low, rs[...])))
    loads[6].wait()
    rt[...] = turn(dot(normed, wr[...]).astype(BF).astype(F32))
    start_fetches(2)
    loads[7].start()

    block = math.gcd(count, 8)
    ones = jnp.ones((width, width), BF)
    lane = lax.broadcasted_iota(jnp.int32, (width, lanes), 1)

    def dot_split(values, right):
        flat = values.reshape(-1, values.shape[-1])
        high = flat.astype(BF)
        low = (flat - high.astype(F32)).astype(BF)
        return dot(high, right) + dot(low, right)

    def one_head(h, c):
        fetch(h).wait()
        k = kh[h]
        d = dh[h]
        unit = k * lax.rsqrt(jnp.sum(k * k, axis=-1, keepdims=True) + 1e-06)
        ua = unit * ah[h]
        rows = pl.ds(pl.multiple_of(h * width, width), width)
        v = vt[rows, :]
        r = rt[rows, :].astype(BF)
        tall = jnp.concatenate([k, jnp.zeros((lanes - count, width), F32)], axis=0).astype(BF)
        mixed = jnp.zeros((width, lanes), F32)
        for g in range(count // block):
            some = range(g * block, (g + 1) * block)

            def each(values):
                return jnp.stack([jnp.broadcast_to(values[b:b + 1], (width, width)) for b in some])

            s = st[h, g * block:(g + 1) * block]
            probe = dot_split(s * each(unit), ones).reshape(block, width, width)
            masked = jnp.concatenate([jnp.where(lane == b, v, 0.0) for b in some], axis=0)
            outer = dot(masked.astype(BF), tall).reshape(block, width, width)
            new = s * each(d) - probe * each(ua) + outer
            st[h, g * block:(g + 1) * block] = new
            got = dot_split(new, r).reshape(block, width, lanes)
            for i, b in enumerate(some):
                mixed = jnp.where(lane == b, got[i], mixed)
        put(h).start()
        centre = mixed - jnp.mean(mixed, axis=0, keepdims=True)
        var = jnp.mean(centre * centre, axis=0, keepdims=True)
        mt[rows, :] = centre * lax.rsqrt(var + 0.00064)
        return c

    lax.fori_loop(0, heads, one_head, 0)
    mixed = (mt[...].T[:count] * head_gain[...]).astype(BF)
    loads[7].wait()
    after = resid + dot(mixed, wo[...])
    after_ref[...] = after
    mean_sq = jnp.mean(after * after, axis=-1, keepdims=True)
    second = (after * lax.rsqrt(mean_sq + 1e-06) * second_gain[...]).astype(BF)
    part = second.shape[1] // (PARTS + 1)
    last = second[:, PARTS * part:]
    for j in range(PARTS):
        value = dot(table[PARTS], second[:, j * part:(j + 1) * part]) + dot(table[j], last)
        packed_ref[:, :, j * part:(j + 1) * part] = value.reshape(EXPERTS, ROWS, part).astype(BF)

    def end_put(h, c):
        put(h).wait()
        return c

    lax.fori_loop(0, heads, end_put, 0)


def mixer(args, table):
    (tokens, state, norm_gain, w_recept, w_keys, w_values, decay_base, d_first, d_second,
     rate_base, r_first, r_second, head_gain, w_output, second_gain) = args
    count, heads, width, _ = state.shape
    model = tokens.shape[1]
    part = model // (PARTS + 1)
    lanes = -(-count // 128) * 128
    vm = pl.BlockSpec(memory_space=pltpu.VMEM)
    hb = pl.BlockSpec(memory_space=pl.ANY)
    weights = [w_recept, w_keys, w_values, d_first, d_second, r_first, r_second, w_output]
    head_buf = pltpu.VMEM((heads, count, width), F32)
    return pl.pallas_call(
        mixer_kernel,
        out_shape=(
            jax.ShapeDtypeStruct(state.shape, F32),
            jax.ShapeDtypeStruct((count, model), F32),
            jax.ShapeDtypeStruct((EXPERTS, ROWS, PARTS * part), BF),
        ),
        in_specs=[vm] * 7 + [hb] * 9,
        out_specs=(hb, vm, vm),
        scratch_shapes=[
            pltpu.VMEM((heads, count, width, width), F32),
            *[pltpu.VMEM(w.shape, w.dtype) for w in weights],
            head_buf, head_buf, head_buf,
            pltpu.VMEM((heads * width, lanes), F32),
            pltpu.VMEM((heads * width, lanes), F32),
            pltpu.VMEM((heads * width, lanes), F32),
            pltpu.SemaphoreType.DMA((8,)),
            pltpu.SemaphoreType.DMA((heads,)),
            pltpu.SemaphoreType.DMA((heads,)),
        ],
        compiler_params=pltpu.CompilerParams(vmem_limit_bytes=56 * 1024 * 1024),
        name="mixer",
    )(
        tokens, norm_gain[None], decay_base[None], rate_base[None], head_gain[None],
        second_gain[None], table, state, *weights,
    )


def expert_kernel(
    devices, packed, after, blend_w, unpack_m, pack_m, gate_h, up_h, down_h,
    out_ref,
    buf, rows_x, hidden, part_f, part_b, peer_b, zsend, ret, gate, up, down,
    w_sem, send1, recv1, fsend, frecv, ysend, yrecv, rsend, rrecv, own_sem,
):
    group = devices // EXPERTS
    me = lax.axis_index("ep")
    mine = me // group
    place = lax.rem(me, group)
    model = after.shape[1]
    part = model // (PARTS + 1)
    inner = gate.shape[1]
    step = math.gcd(inner, 256)

    loads = [
        pltpu.make_async_copy(src, dst, w_sem.at[i])
        for i, (src, dst) in enumerate([(gate_h, gate), (up_h, up), (down_h, down)])
    ]
    barrier = pltpu.get_barrier_semaphore()

    def other(i):
        return lax.rem(mine + i, EXPERTS)

    def peer(i):
        return lax.rem(place + i, group)

    def greet(i, c):
        pl.semaphore_signal(
            barrier, inc=1, device_id=(other(i) * group + place,), device_id_type=MESH
        )
        return c

    lax.fori_loop(1, EXPERTS, greet, 0)
    for i in range(1, group):
        pl.semaphore_signal(
            barrier, inc=1, device_id=(mine * group + peer(i),), device_id_type=MESH
        )
    for copy in loads:
        copy.start()
    pl.semaphore_wait(barrier, EXPERTS - 1 + group - 1)

    def dispatch(i):
        e = other(i)
        return pltpu.make_async_remote_copy(
            src_ref=packed.at[e], dst_ref=buf.at[place, mine],
            send_sem=send1.at[e], recv_sem=recv1.at[mine],
            device_id=(e * group + place,), device_id_type=MESH,
        )

    def arrive(s):
        return pltpu.make_async_remote_copy(
            src_ref=packed.at[s], dst_ref=buf.at[place, s],
            send_sem=send1.at[s], recv_sem=recv1.at[s],
            device_id=(s * group + place,), device_id_type=MESH,
        )

    def forward(s, i, src):
        q = peer(i)
        return pltpu.make_async_remote_copy(
            src_ref=src, dst_ref=buf.at[place, s],
            send_sem=fsend.at[i, s], recv_sem=frecv.at[place, s],
            device_id=(mine * group + q,), device_id_type=MESH,
        )

    def forwarded(s, i):
        q = peer(i)
        return pltpu.make_async_remote_copy(
            src_ref=buf.at[q, s], dst_ref=buf.at[q, s],
            send_sem=fsend.at[i, s], recv_sem=frecv.at[q, s],
            device_id=(mine * group + q,), device_id_type=MESH,
        )

    def start_dispatch(i, c):
        dispatch(i).start()
        return c

    lax.fori_loop(1, EXPERTS, start_dispatch, 0)
    own = pltpu.make_async_copy(packed.at[mine], buf.at[place, mine], own_sem.at[0])
    own.start()
    for i in range(1, group):
        forward(mine, i, packed.at[mine]).start()

    def relay(j, c):
        s = lax.rem(mine + EXPERTS - j, EXPERTS)
        arrive(s).wait_recv()
        for i in range(1, group):
            forward(s, i, buf.at[place, s]).start()
        return c

    lax.fori_loop(1, EXPERTS, relay, 0)
    own.wait()

    def end_relay(j, c):
        s = lax.rem(mine + EXPERTS - j, EXPERTS)
        for i in range(1, group):
            forwarded(s, i).wait_recv()
        return c

    lax.fori_loop(0, EXPERTS, end_relay, 0)

    packed_rows = EXPERTS * ROWS
    rows = EXPERTS * CAP_DEV
    for q in range(group):
        tail = jnp.zeros((rows, part), F32)
        for j in range(PARTS):
            cols = slice(j * part, (j + 1) * part)
            block = buf[q, :, :, cols].astype(F32).reshape(packed_rows, part).astype(BF)
            rows_x[q * rows:(q + 1) * rows, cols] = dot(unpack_m[PARTS], block).astype(BF)
            tail = tail + dot(unpack_m[j], block)
        rows_x[q * rows:(q + 1) * rows, PARTS * part:] = tail.astype(BF)

    loads[0].wait()
    loads[1].wait()

    def up_step(t, c):
        cols = pl.ds(pl.multiple_of(t * step, step), step)
        g = dot(rows_x[...], gate[:, cols])
        u = dot(rows_x[...], up[:, cols])
        hidden[:, cols] = (g * jax.nn.sigmoid(g) * u).astype(BF)
        return c

    lax.fori_loop(0, inner // step, up_step, 0)
    loads[2].wait()
    wide = math.gcd(model, 256)

    def down_step(t, c):
        cols = pl.ds(pl.multiple_of(t * wide, wide), wide)
        y = dot(hidden[...], down[:, cols])
        for q in range(group):
            mine_rows = y[q * rows:(q + 1) * rows]
            part_f[q, :, cols] = mine_rows
            part_b[q, :, cols] = mine_rows.astype(BF)
        return c

    lax.fori_loop(0, model // wide, down_step, 0)

    def swap(i):
        q = peer(i)
        return pltpu.make_async_remote_copy(
            src_ref=part_b.at[q], dst_ref=peer_b.at[place],
            send_sem=ysend.at[q], recv_sem=yrecv.at[place],
            device_id=(mine * group + q,), device_id_type=MESH,
        )

    def swapped(i):
        q = peer(i)
        return pltpu.make_async_remote_copy(
            src_ref=part_b.at[q], dst_ref=peer_b.at[q],
            send_sem=ysend.at[q], recv_sem=yrecv.at[q],
            device_id=(mine * group + q,), device_id_type=MESH,
        )

    for i in range(1, group):
        swap(i).start()
    for i in range(1, group):
        swapped(i).wait_recv()

    def summed(cols):
        total = part_f[place, :, cols]
        for i in range(1, group):
            total = total + peer_b[peer(i), :, cols].astype(F32)
        return total.astype(BF)

    last = summed(slice(PARTS * part, model))
    for j in range(PARTS):
        cols = slice(j * part, (j + 1) * part)
        value = dot(pack_m[PARTS], summed(cols)) + dot(pack_m[j], last)
        zsend[:, :, cols] = value.reshape(EXPERTS, ROWS, part).astype(BF)

    def give(i):
        e = other(i)
        return pltpu.make_async_remote_copy(
            src_ref=zsend.at[e], dst_ref=ret.at[mine],
            send_sem=rsend.at[e], recv_sem=rrecv.at[mine],
            device_id=(e * group + place,), device_id_type=MESH,
        )

    def take(s):
        return pltpu.make_async_remote_copy(
            src_ref=zsend.at[s], dst_ref=ret.at[s],
            send_sem=rsend.at[s], recv_sem=rrecv.at[s],
            device_id=(s * group + place,), device_id_type=MESH,
        )

    def start_give(i, c):
        give(i).start()
        return c

    lax.fori_loop(1, EXPERTS, start_give, 0)
    own_back = pltpu.make_async_copy(zsend.at[mine], ret.at[mine], own_sem.at[1])
    own_back.start()

    def drain(i, c):
        dispatch(i).wait_send()
        s = lax.rem(mine + EXPERTS - i, EXPERTS)
        for k in range(1, group):
            forwarded(s, k).wait_send()
        return c

    lax.fori_loop(1, EXPERTS, drain, 0)
    for i in range(1, group):
        forwarded(mine, i).wait_send()
        swap(i).wait_send()
    own_back.wait()

    def end_take(j, c):
        take(lax.rem(mine + EXPERTS - j, EXPERTS)).wait_recv()
        return c

    lax.fori_loop(1, EXPERTS, end_take, 0)

    high = blend_w[...].astype(BF)
    low = (blend_w[...] - high.astype(F32)).astype(BF)
    tail = after[:, PARTS * part:]
    for j in range(PARTS):
        cols = slice(j * part, (j + 1) * part)
        block = ret[:, :, cols].astype(F32).reshape(packed_rows, part).astype(BF)
        value = after[:, cols] + dot(high[PARTS], block) + dot(low[PARTS], block)
        out_ref[:, cols] = value.astype(BF)
        tail = tail + dot(high[j], block) + dot(low[j], block)
    out_ref[:, PARTS * part:] = tail.astype(BF)

    def end_give(i, c):
        give(i).wait_send()
        return c

    lax.fori_loop(1, EXPERTS, end_give, 0)


def experts(packed, after, blend_w, gate, up, down, devices):
    group = devices // EXPERTS
    count, model = after.shape
    inner = gate.shape[1]
    rows = EXPERTS * CAP_DEV
    row = np.arange(rows)[:, None]
    place = np.arange(EXPERTS * ROWS)[None, :]
    same = row // CAP_DEV == place // ROWS
    slot, at = row % CAP_DEV, place % ROWS
    maps = [
        same & (at == CAP_DEV + slot // PARTS) & (slot % PARTS == j) for j in range(PARTS)
    ] + [same & (at == slot)]
    maps = np.stack(maps).astype(np.float32)
    unpack_m = jnp.asarray(maps, BF)
    pack_m = jnp.asarray(maps.transpose(0, 2, 1), BF)
    vm = pl.BlockSpec(memory_space=pltpu.VMEM)
    hb = pl.BlockSpec(memory_space=pl.ANY)
    wide = packed.shape[2]
    dma = pltpu.SemaphoreType.DMA
    return pl.pallas_call(
        functools.partial(expert_kernel, devices),
        out_shape=jax.ShapeDtypeStruct((count, model), BF),
        in_specs=[vm] * 5 + [hb] * 3,
        out_specs=vm,
        scratch_shapes=[
            pltpu.VMEM((group, EXPERTS, ROWS, wide), BF),
            pltpu.VMEM((group * rows, model), BF),
            pltpu.VMEM((group * rows, inner), BF),
            pltpu.VMEM((group, rows, model), F32),
            pltpu.VMEM((group, rows, model), BF),
            pltpu.VMEM((group, rows, model), BF),
            pltpu.VMEM((EXPERTS, ROWS, wide), BF),
            pltpu.VMEM((EXPERTS, ROWS, wide), BF),
            pltpu.VMEM(gate.shape, BF),
            pltpu.VMEM(up.shape, BF),
            pltpu.VMEM(down.shape, BF),
            dma((3,)),
            dma((EXPERTS,)),
            dma((EXPERTS,)),
            dma((group, EXPERTS)),
            dma((group, EXPERTS)),
            dma((group,)),
            dma((group,)),
            dma((EXPERTS,)),
            dma((EXPERTS,)),
            dma((2,)),
        ],
        compiler_params=pltpu.CompilerParams(
            collective_id=0, has_side_effects=True, vmem_limit_bytes=56 * 1024 * 1024
        ),
        name="experts",
    )(packed, after, blend_w, unpack_m, pack_m, gate, up, down)


def tables(route_ids, route_weights, rows_dev):
    start = lax.axis_index("ep") * rows_dev
    ids = lax.dynamic_slice_in_dim(route_ids, start, rows_dev, 0)
    weights = lax.dynamic_slice_in_dim(route_weights, start, rows_dev, 0)
    hit = ids[None, :, :] == jnp.arange(EXPERTS, dtype=jnp.int32)[:, None, None]
    member = jnp.any(hit, axis=2)
    share = jnp.sum(jnp.where(hit, weights[None, :, :], 0.0), axis=2)
    order = jnp.cumsum(member.astype(jnp.int32), axis=1) - 1
    order = jnp.where(member, order, -1)[None, :, None, :]
    at = np.arange(ROWS)[None, None, :, None]
    piece = np.arange(PARTS + 1)[:, None, None, None]
    base = np.where(
        piece == PARTS,
        np.where(at < CAP_DEV, at, -2),
        np.where(at >= CAP_DEV, (at - CAP_DEV) * PARTS + piece, -2),
    ).astype(np.int32)
    table = (order == base).astype(F32)
    blend = table * share[None, :, None, :]
    flat = (PARTS + 1, EXPERTS * ROWS, rows_dev)
    return table.reshape(flat).astype(BF), blend.reshape(flat).transpose(0, 2, 1)


def on_device(
    tokens, state, norm_gain, w_recept, w_keys, w_values, decay_base, decay_first_matrix,
    decay_second_matrix, rate_base, rate_first_matrix, rate_second_matrix, head_gain, w_output,
    second_gain, route_ids, route_weights, expert_gate, expert_up, expert_down,
):
    devices = lax.axis_size("ep")
    table, blend_w = tables(route_ids, route_weights, tokens.shape[0])
    new_state, after, packed = mixer(
        (tokens, state, norm_gain, w_recept, w_keys, w_values, decay_base, decay_first_matrix,
         decay_second_matrix, rate_base, rate_first_matrix, rate_second_matrix, head_gain,
         w_output, second_gain),
        table,
    )
    layer_out = experts(packed, after, blend_w, expert_gate, expert_up, expert_down, devices)
    return (layer_out, new_state)


def solution(mesh):
    rep = P()
    in_specs = (
        P("ep", None), P("ep", None, None, None), *[rep] * 15,
        P(None, "ep"), P(None, "ep"), P("ep", None),
    )
    out_specs = (P("ep", None), P("ep", None, None, None))
    return jax.shard_map(
        on_device, mesh=mesh, in_specs=in_specs, out_specs=out_specs, check_vma=False
    )
```

```python
import functools
import math

import jax
import jax.numpy as jnp
import numpy as np
from jax import lax
from jax.experimental import pallas as pl
from jax.experimental.pallas import tpu as pltpu
from jax.sharding import PartitionSpec as P

EXPERTS = 16
CAP_DEV = 6
ROWS = 8
PARTS = 3
MESH = pl.DeviceIdType.MESH
BF = jnp.bfloat16
F32 = jnp.float32


def dot(a, b):
    return jnp.dot(a, b, preferred_element_type=F32)


def mixer_kernel(
    tokens, norm_gain, decay_base, rate_base, head_gain, second_gain, order, share,
    state, w_recept, w_keys, w_values, d_first, d_second, r_first, r_second, w_output,
    new_state, after_ref, packed_ref, blend_ref,
    st, wr, wk, wv, df, ds, rf, rs, wo, kh, dh, ah, vt, rt, mt,
    w_sem, in_sem, out_sem,
):
    count, heads, width, _ = state.shape
    loads = [
        pltpu.make_async_copy(src, dst, w_sem.at[i])
        for i, (src, dst) in enumerate(
            [
                (d_first, df), (r_first, rf), (w_keys, wk), (w_values, wv), (d_second, ds),
                (r_second, rs), (w_recept, wr), (w_output, wo),
            ]
        )
    ]
    for copy in loads[:7]:
        copy.start()

    def fetch(h):
        return pltpu.make_async_copy(state.at[:, h], st.at[h], in_sem.at[h])

    def put(h):
        return pltpu.make_async_copy(st.at[h], new_state.at[:, h], out_sem.at[h])

    def start_fetch(h, c):
        fetch(h).start()
        return c

    def start_fetches(turn_at):
        low, high = turn_at * heads // 3, (turn_at + 1) * heads // 3
        lax.fori_loop(low, high, start_fetch, 0)

    shape = (EXPERTS, ROWS, count)
    slot = jnp.broadcast_to(order[...][:, None, :], shape)
    weight = jnp.broadcast_to(share[...][:, None, :], shape)
    at = lax.broadcasted_iota(jnp.int32, shape, 1)
    table = []
    for j in range(PARTS + 1):
        if j == PARTS:
            hits = (slot == at) & (at < CAP_DEV)
        else:
            hits = (slot == (at - CAP_DEV) * PARTS + j) & (at >= CAP_DEV)
        hits = jnp.where(hits, 1.0, 0.0)
        blend_ref[j] = (hits * weight).reshape(EXPERTS * ROWS, count)
        table.append(hits.reshape(EXPERTS * ROWS, count).astype(BF))

    resid = tokens[...].astype(F32)
    mean_sq = jnp.mean(resid * resid, axis=-1, keepdims=True)
    normed = (resid * lax.rsqrt(mean_sq + 1e-06) * norm_gain[...]).astype(BF)

    def spread(ref, values):
        for h in range(heads):
            ref[h] = values[:, h * width:(h + 1) * width]

    lanes = vt.shape[1]

    def turn(values):
        blank = jnp.zeros((lanes - count, values.shape[1]), F32)
        return jnp.concatenate([values, blank], axis=0).T

    loads[0].wait()
    decay_low = jnp.tanh(dot(normed, df[...])).astype(BF)
    loads[1].wait()
    rate_low = dot(normed, rf[...]).astype(BF)
    loads[2].wait()
    spread(kh, dot(normed, wk[...]).astype(BF).astype(F32))
    start_fetches(0)
    loads[3].wait()
    vals = dot(normed, wv[...]).astype(BF).astype(F32)
    vt[...] = turn(vals)
    start_fetches(1)
    loads[4].wait()
    pre = decay_base[...] + dot(decay_low, ds[...])
    spread(dh, jnp.exp(-jax.nn.sigmoid(pre) * math.exp(-0.5)))
    loads[5].wait()
    spread(ah, jax.nn.sigmoid(rate_base[...] + dot(rate_low, rs[...])))
    loads[6].wait()
    rt[...] = turn(dot(normed, wr[...]).astype(BF).astype(F32))
    start_fetches(2)
    loads[7].start()

    block = math.gcd(count, 8)
    ones = jnp.ones((width, width), BF)
    lane = lax.broadcasted_iota(jnp.int32, (width, lanes), 1)

    def dot_split(values, right):
        flat = values.reshape(-1, values.shape[-1])
        high = flat.astype(BF)
        low = (flat - high.astype(F32)).astype(BF)
        return dot(high, right) + dot(low, right)

    def one_head(h, c):
        fetch(h).wait()
        k = kh[h]
        d = dh[h]
        unit = k * lax.rsqrt(jnp.sum(k * k, axis=-1, keepdims=True) + 1e-06)
        ua = unit * ah[h]
        rows = pl.ds(pl.multiple_of(h * width, width), width)
        v = vt[rows, :]
        r = rt[rows, :].astype(BF)
        tall = jnp.concatenate([k, jnp.zeros((lanes - count, width), F32)], axis=0).astype(BF)
        mixed = jnp.zeros((width, lanes), F32)
        for g in range(count // block):
            some = range(g * block, (g + 1) * block)

            def each(values):
                return jnp.stack([jnp.broadcast_to(values[b:b + 1], (width, width)) for b in some])

            s = st[h, g * block:(g + 1) * block]
            probe = dot_split(s * each(unit), ones).reshape(block, width, width)
            masked = jnp.concatenate([jnp.where(lane == b, v, 0.0) for b in some], axis=0)
            outer = dot(masked.astype(BF), tall).reshape(block, width, width)
            new = s * each(d) - probe * each(ua) + outer
            st[h, g * block:(g + 1) * block] = new
            got = dot_split(new, r).reshape(block, width, lanes)
            for i, b in enumerate(some):
                mixed = jnp.where(lane == b, got[i], mixed)
        put(h).start()
        centre = mixed - jnp.mean(mixed, axis=0, keepdims=True)
        var = jnp.mean(centre * centre, axis=0, keepdims=True)
        mt[rows, :] = centre * lax.rsqrt(var + 0.00064)
        return c

    lax.fori_loop(0, heads, one_head, 0)
    mixed = (mt[...].T[:count] * head_gain[...]).astype(BF)
    loads[7].wait()
    after = resid + dot(mixed, wo[...])
    after_ref[...] = after
    mean_sq = jnp.mean(after * after, axis=-1, keepdims=True)
    second = (after * lax.rsqrt(mean_sq + 1e-06) * second_gain[...]).astype(BF)
    part = second.shape[1] // (PARTS + 1)
    last = second[:, PARTS * part:]
    for j in range(PARTS):
        value = dot(table[PARTS], second[:, j * part:(j + 1) * part]) + dot(table[j], last)
        packed_ref[:, :, j * part:(j + 1) * part] = value.reshape(EXPERTS, ROWS, part).astype(BF)

    def end_put(h, c):
        put(h).wait()
        return c

    lax.fori_loop(0, heads, end_put, 0)


def mixer(args, order, share):
    (tokens, state, norm_gain, w_recept, w_keys, w_values, decay_base, d_first, d_second,
     rate_base, r_first, r_second, head_gain, w_output, second_gain) = args
    count, heads, width, _ = state.shape
    model = tokens.shape[1]
    part = model // (PARTS + 1)
    lanes = -(-count // 128) * 128
    vm = pl.BlockSpec(memory_space=pltpu.VMEM)
    hb = pl.BlockSpec(memory_space=pl.ANY)
    weights = [w_recept, w_keys, w_values, d_first, d_second, r_first, r_second, w_output]
    head_buf = pltpu.VMEM((heads, count, width), F32)
    return pl.pallas_call(
        mixer_kernel,
        out_shape=(
            jax.ShapeDtypeStruct(state.shape, F32),
            jax.ShapeDtypeStruct((count, model), F32),
            jax.ShapeDtypeStruct((EXPERTS, ROWS, PARTS * part), BF),
            jax.ShapeDtypeStruct((PARTS + 1, EXPERTS * ROWS, count), F32),
        ),
        in_specs=[vm] * 8 + [hb] * 9,
        out_specs=(hb, vm, vm, vm),
        scratch_shapes=[
            pltpu.VMEM((heads, count, width, width), F32),
            *[pltpu.VMEM(w.shape, w.dtype) for w in weights],
            head_buf, head_buf, head_buf,
            pltpu.VMEM((heads * width, lanes), F32),
            pltpu.VMEM((heads * width, lanes), F32),
            pltpu.VMEM((heads * width, lanes), F32),
            pltpu.SemaphoreType.DMA((8,)),
            pltpu.SemaphoreType.DMA((heads,)),
            pltpu.SemaphoreType.DMA((heads,)),
        ],
        compiler_params=pltpu.CompilerParams(vmem_limit_bytes=56 * 1024 * 1024),
        name="mixer",
    )(
        tokens, norm_gain[None], decay_base[None], rate_base[None], head_gain[None],
        second_gain[None], order, share, state, *weights,
    )


def expert_kernel(
    devices, packed, after, blend_w, unpack_m, pack_m, gate_h, up_h, down_h,
    out_ref,
    buf, rows_x, hidden, part_f, part_b, peer_b, zsend, ret, gate, up, down,
    w_sem, send1, recv1, fsend, frecv, ysend, yrecv, rsend, rrecv, own_sem,
):
    group = devices // EXPERTS
    me = lax.axis_index("ep")
    mine = me // group
    place = lax.rem(me, group)
    model = after.shape[1]
    part = model // (PARTS + 1)
    inner = gate.shape[1]
    step = math.gcd(inner, 256)

    loads = [
        pltpu.make_async_copy(src, dst, w_sem.at[i])
        for i, (src, dst) in enumerate([(gate_h, gate), (up_h, up), (down_h, down)])
    ]
    barrier = pltpu.get_barrier_semaphore()

    def other(i):
        return lax.rem(mine + i, EXPERTS)

    def peer(i):
        return lax.rem(place + i, group)

    def greet(i, c):
        pl.semaphore_signal(
            barrier, inc=1, device_id=(other(i) * group + place,), device_id_type=MESH
        )
        return c

    lax.fori_loop(1, EXPERTS, greet, 0)
    for i in range(1, group):
        pl.semaphore_signal(
            barrier, inc=1, device_id=(mine * group + peer(i),), device_id_type=MESH
        )
    for copy in loads:
        copy.start()
    pl.semaphore_wait(barrier, EXPERTS - 1 + group - 1)

    def dispatch(i):
        e = other(i)
        return pltpu.make_async_remote_copy(
            src_ref=packed.at[e], dst_ref=buf.at[place, mine],
            send_sem=send1.at[e], recv_sem=recv1.at[mine],
            device_id=(e * group + place,), device_id_type=MESH,
        )

    def arrive(s):
        return pltpu.make_async_remote_copy(
            src_ref=packed.at[s], dst_ref=buf.at[place, s],
            send_sem=send1.at[s], recv_sem=recv1.at[s],
            device_id=(s * group + place,), device_id_type=MESH,
        )

    def forward(s, i, src):
        q = peer(i)
        return pltpu.make_async_remote_copy(
            src_ref=src, dst_ref=buf.at[place, s],
            send_sem=fsend.at[i, s], recv_sem=frecv.at[place, s],
            device_id=(mine * group + q,), device_id_type=MESH,
        )

    def forwarded(s, i):
        q = peer(i)
        return pltpu.make_async_remote_copy(
            src_ref=buf.at[q, s], dst_ref=buf.at[q, s],
            send_sem=fsend.at[i, s], recv_sem=frecv.at[q, s],
            device_id=(mine * group + q,), device_id_type=MESH,
        )

    def start_dispatch(i, c):
        dispatch(i).start()
        return c

    lax.fori_loop(1, EXPERTS, start_dispatch, 0)
    own = pltpu.make_async_copy(packed.at[mine], buf.at[place, mine], own_sem.at[0])
    own.start()
    for i in range(1, group):
        forward(mine, i, packed.at[mine]).start()

    def relay(j, c):
        s = lax.rem(mine + EXPERTS - j, EXPERTS)
        arrive(s).wait_recv()
        for i in range(1, group):
            forward(s, i, buf.at[place, s]).start()
        return c

    lax.fori_loop(1, EXPERTS, relay, 0)
    own.wait()

    def end_relay(j, c):
        s = lax.rem(mine + EXPERTS - j, EXPERTS)
        for i in range(1, group):
            forwarded(s, i).wait_recv()
        return c

    lax.fori_loop(0, EXPERTS, end_relay, 0)

    packed_rows = EXPERTS * ROWS
    rows = EXPERTS * CAP_DEV
    for q in range(group):
        tail = jnp.zeros((rows, part), F32)
        for j in range(PARTS):
            cols = slice(j * part, (j + 1) * part)
            block = buf[q, :, :, cols].astype(F32).reshape(packed_rows, part).astype(BF)
            rows_x[q * rows:(q + 1) * rows, cols] = dot(unpack_m[PARTS], block).astype(BF)
            tail = tail + dot(unpack_m[j], block)
        rows_x[q * rows:(q + 1) * rows, PARTS * part:] = tail.astype(BF)

    loads[0].wait()
    loads[1].wait()

    def up_step(t, c):
        cols = pl.ds(pl.multiple_of(t * step, step), step)
        g = dot(rows_x[...], gate[:, cols])
        u = dot(rows_x[...], up[:, cols])
        hidden[:, cols] = (g * jax.nn.sigmoid(g) * u).astype(BF)
        return c

    lax.fori_loop(0, inner // step, up_step, 0)
    loads[2].wait()
    wide = math.gcd(model, 256)

    def down_step(t, c):
        cols = pl.ds(pl.multiple_of(t * wide, wide), wide)
        y = dot(hidden[...], down[:, cols])
        for q in range(group):
            mine_rows = y[q * rows:(q + 1) * rows]
            part_f[q, :, cols] = mine_rows
            part_b[q, :, cols] = mine_rows.astype(BF)
        return c

    lax.fori_loop(0, model // wide, down_step, 0)

    def swap(i):
        q = peer(i)
        return pltpu.make_async_remote_copy(
            src_ref=part_b.at[q], dst_ref=peer_b.at[place],
            send_sem=ysend.at[q], recv_sem=yrecv.at[place],
            device_id=(mine * group + q,), device_id_type=MESH,
        )

    def swapped(i):
        q = peer(i)
        return pltpu.make_async_remote_copy(
            src_ref=part_b.at[q], dst_ref=peer_b.at[q],
            send_sem=ysend.at[q], recv_sem=yrecv.at[q],
            device_id=(mine * group + q,), device_id_type=MESH,
        )

    for i in range(1, group):
        swap(i).start()
    for i in range(1, group):
        swapped(i).wait_recv()

    def summed(cols):
        total = part_f[place, :, cols]
        for i in range(1, group):
            total = total + peer_b[peer(i), :, cols].astype(F32)
        return total.astype(BF)

    last = summed(slice(PARTS * part, model))
    for j in range(PARTS):
        cols = slice(j * part, (j + 1) * part)
        value = dot(pack_m[PARTS], summed(cols)) + dot(pack_m[j], last)
        zsend[:, :, cols] = value.reshape(EXPERTS, ROWS, part).astype(BF)

    def give(i):
        e = other(i)
        return pltpu.make_async_remote_copy(
            src_ref=zsend.at[e], dst_ref=ret.at[mine],
            send_sem=rsend.at[e], recv_sem=rrecv.at[mine],
            device_id=(e * group + place,), device_id_type=MESH,
        )

    def take(s):
        return pltpu.make_async_remote_copy(
            src_ref=zsend.at[s], dst_ref=ret.at[s],
            send_sem=rsend.at[s], recv_sem=rrecv.at[s],
            device_id=(s * group + place,), device_id_type=MESH,
        )

    def start_give(i, c):
        give(i).start()
        return c

    lax.fori_loop(1, EXPERTS, start_give, 0)
    own_back = pltpu.make_async_copy(zsend.at[mine], ret.at[mine], own_sem.at[1])
    own_back.start()

    def drain(i, c):
        dispatch(i).wait_send()
        s = lax.rem(mine + EXPERTS - i, EXPERTS)
        for k in range(1, group):
            forwarded(s, k).wait_send()
        return c

    lax.fori_loop(1, EXPERTS, drain, 0)
    for i in range(1, group):
        forwarded(mine, i).wait_send()
        swap(i).wait_send()
    own_back.wait()

    def end_take(j, c):
        take(lax.rem(mine + EXPERTS - j, EXPERTS)).wait_recv()
        return c

    lax.fori_loop(1, EXPERTS, end_take, 0)

    def dot_turned(left, right):
        return lax.dot_general(left, right, (((0,), (0,)), ((), ())), preferred_element_type=F32)

    high = blend_w[...].astype(BF)
    low = (blend_w[...] - high.astype(F32)).astype(BF)
    tail = after[:, PARTS * part:]
    for j in range(PARTS):
        cols = slice(j * part, (j + 1) * part)
        block = ret[:, :, cols].astype(F32).reshape(packed_rows, part).astype(BF)
        value = after[:, cols] + dot_turned(high[PARTS], block) + dot_turned(low[PARTS], block)
        out_ref[:, cols] = value.astype(BF)
        tail = tail + dot_turned(high[j], block) + dot_turned(low[j], block)
    out_ref[:, PARTS * part:] = tail.astype(BF)

    def end_give(i, c):
        give(i).wait_send()
        return c

    lax.fori_loop(1, EXPERTS, end_give, 0)


def experts(packed, after, blend_w, gate, up, down, devices):
    group = devices // EXPERTS
    count, model = after.shape
    inner = gate.shape[1]
    rows = EXPERTS * CAP_DEV
    row = np.arange(rows)[:, None]
    place = np.arange(EXPERTS * ROWS)[None, :]
    same = row // CAP_DEV == place // ROWS
    slot, at = row % CAP_DEV, place % ROWS
    maps = [
        same & (at == CAP_DEV + slot // PARTS) & (slot % PARTS == j) for j in range(PARTS)
    ] + [same & (at == slot)]
    maps = np.stack(maps).astype(np.float32)
    unpack_m = jnp.asarray(maps, BF)
    pack_m = jnp.asarray(maps.transpose(0, 2, 1), BF)
    vm = pl.BlockSpec(memory_space=pltpu.VMEM)
    hb = pl.BlockSpec(memory_space=pl.ANY)
    wide = packed.shape[2]
    dma = pltpu.SemaphoreType.DMA
    return pl.pallas_call(
        functools.partial(expert_kernel, devices),
        out_shape=jax.ShapeDtypeStruct((count, model), BF),
        in_specs=[vm] * 5 + [hb] * 3,
        out_specs=vm,
        scratch_shapes=[
            pltpu.VMEM((group, EXPERTS, ROWS, wide), BF),
            pltpu.VMEM((group * rows, model), BF),
            pltpu.VMEM((group * rows, inner), BF),
            pltpu.VMEM((group, rows, model), F32),
            pltpu.VMEM((group, rows, model), BF),
            pltpu.VMEM((group, rows, model), BF),
            pltpu.VMEM((EXPERTS, ROWS, wide), BF),
            pltpu.VMEM((EXPERTS, ROWS, wide), BF),
            pltpu.VMEM(gate.shape, BF),
            pltpu.VMEM(up.shape, BF),
            pltpu.VMEM(down.shape, BF),
            dma((3,)),
            dma((EXPERTS,)),
            dma((EXPERTS,)),
            dma((group, EXPERTS)),
            dma((group, EXPERTS)),
            dma((group,)),
            dma((group,)),
            dma((EXPERTS,)),
            dma((EXPERTS,)),
            dma((2,)),
        ],
        compiler_params=pltpu.CompilerParams(
            collective_id=0, has_side_effects=True, vmem_limit_bytes=56 * 1024 * 1024
        ),
        name="experts",
    )(packed, after, blend_w, unpack_m, pack_m, gate, up, down)


def tables(route_ids, route_weights, rows_dev):
    start = lax.axis_index("ep") * rows_dev
    ids = lax.dynamic_slice_in_dim(route_ids, start, rows_dev, 0)
    weights = lax.dynamic_slice_in_dim(route_weights, start, rows_dev, 0)
    hit = ids[None, :, :] == jnp.arange(EXPERTS, dtype=jnp.int32)[:, None, None]
    member = jnp.any(hit, axis=2)
    share = jnp.sum(jnp.where(hit, weights[None, :, :], 0.0), axis=2)
    order = jnp.cumsum(member.astype(jnp.int32), axis=1) - 1
    return jnp.where(member, order, -1), share


def on_device(
    tokens, state, norm_gain, w_recept, w_keys, w_values, decay_base, decay_first_matrix,
    decay_second_matrix, rate_base, rate_first_matrix, rate_second_matrix, head_gain, w_output,
    second_gain, route_ids, route_weights, expert_gate, expert_up, expert_down,
):
    devices = lax.axis_size("ep")
    order, share = tables(route_ids, route_weights, tokens.shape[0])
    new_state, after, packed, blend_w = mixer(
        (tokens, state, norm_gain, w_recept, w_keys, w_values, decay_base, decay_first_matrix,
         decay_second_matrix, rate_base, rate_first_matrix, rate_second_matrix, head_gain,
         w_output, second_gain),
        order,
        share,
    )
    layer_out = experts(packed, after, blend_w, expert_gate, expert_up, expert_down, devices)
    return (layer_out, new_state)


def solution(mesh):
    rep = P()
    in_specs = (
        P("ep", None), P("ep", None, None, None), *[rep] * 15,
        P(None, "ep"), P(None, "ep"), P("ep", None),
    )
    out_specs = (P("ep", None), P("ep", None, None, None))
    return jax.shard_map(
        on_device, mesh=mesh, in_specs=in_specs, out_specs=out_specs, check_vma=False
    )
```
